32 devices in a mesh: kv: 4 (over y, x), tp: 8 (over z, core).
Axes of the slice: x: 2, y: 2, z: 4, core: 2. Of those that a mesh axis runs over, the one named last changes fastest.
Arguments:
- tokens: bfloat16 [384, 4096], P('kv', 'tp'), may hold values from -20 to 20
- state: float32 [384, 32, 4096], P('kv', 'tp'), may hold values from -4 to 4
- w_query: bfloat16 [4096, 2048], P(None, 'tp'), may hold values from -0.09375 to 0.09375
- w_key: bfloat16 [4096, 2048], P(None, 'tp'), may hold values from -0.09375 to 0.09375
- w_value: bfloat16 [4096, 2048], P(None, 'tp'), may hold values from -0.09375 to 0.09375
- w_gate: bfloat16 [4096, 2048], P(None, 'tp'), may hold values from -0.09375 to 0.09375
- w_decay: bfloat16 [4096, 32], replicated, may hold values from -0.09375 to 0.09375
- w_beta: bfloat16 [4096, 32], replicated, may hold values from -0.09375 to 0.09375
- decay_rate: float32 [32], P('tp'), may hold values from 0.03 to 3
- decay_bias: float32 [32], P('tp'), may hold values from -1 to 1
- mix_gain: float32 [4096], replicated, may hold values from 0.1 to 1.9
- out_gain: float32 [64], replicated, may hold values from 0.1 to 1.9
- w_out: bfloat16 [2048, 4096], P('tp'), may hold values from -0.125 to 0.125
- ffn_gain: float32 [4096], replicated, may hold values from 0.1 to 1.9
- w_up: bfloat16 [4096, 16384], P('tp', 'kv'), may hold values from -0.09375 to 0.09375
- w_down: bfloat16 [16384, 4096], P('kv', 'tp'), may hold values from -0.046875 to 0.046875
Outputs:
- mixed: bfloat16 [384, 4096], P('kv', 'tp')
- new_state: float32 [384, 32, 4096], P('kv', 'tp')
The draws below stay inside these ranges and needn't reach their ends.
All inputs are finite; a program needn't handle non-finite values.
Results may differ from the reference program's by a relative error of at most 0.024.
Values may be sent and summed in bfloat16 or wider, within the bound.
A program may use at most 128 MiB of HBM per device.

```python
import math
import jax
import jax.numpy as jnp
from jax import lax

D = 4096
HEADS = 32
HEAD_DIM = 64
FF = 16384
BATCH = 384


def draw_tokens(key, part):
    scale_key, base_key = jax.random.split(jax.random.fold_in(key, 11))
    scales = jnp.exp(jax.random.uniform(scale_key, (D // 32,), jnp.float32, -1.2, 1.2))
    column_scales = jnp.repeat(scales, 32)
    base = jnp.clip(jax.random.normal(base_key, (BATCH, D), jnp.float32), -6.0, 6.0)
    return (base * column_scales[None, :]).astype(jnp.bfloat16)


def levels(stream_key, shape, cuts, smallest, top_value):
    def one(axis_at, shards_of):
        heights = jax.random.uniform(jax.random.fold_in(jax.random.fold_in(stream_key, 6), axis_at), (shards_of,), jnp.float32, smallest / len(cuts), top_value / len(cuts))
        return jnp.repeat(jnp.exp(heights), shape[axis_at] // shards_of).reshape((-1,) + (1,) * (len(shape) - axis_at - 1))

    gain = one(*cuts[0])
    for cut in cuts[1:]:
        gain = gain * one(*cut)
    return gain


def gaussian(key, shape, scale, limit, cuts=(), kind=jnp.bfloat16):
    level = levels(key, shape, cuts, -0.22, 0.18) if cuts else 1.0
    result = jax.random.normal(key, shape, jnp.float32) * scale * level
    return jnp.minimum(jnp.maximum(result, -limit), limit).astype(kind)


def setup_inputs(seed: int = 0) -> dict:
    splits = jax.random.split(jax.random.key(seed), 17)
    tokens = draw_tokens(jax.random.fold_in(splits[16], 71), 0)
    state = gaussian(splits[1], (BATCH, HEADS, HEAD_DIM * HEAD_DIM), 0.5, 4.0, ((0, 4), (1, 8)), jnp.float32)
    w_query = gaussian(splits[2], (D, HEADS * HEAD_DIM), D ** -0.5, 0.09375, ((1, 8),))
    w_key = gaussian(splits[3], (D, HEADS * HEAD_DIM), D ** -0.5, 0.09375, ((1, 8),))
    w_value = gaussian(splits[4], (D, HEADS * HEAD_DIM), D ** -0.5, 0.09375, ((1, 8),))
    w_gate = gaussian(splits[5], (D, HEADS * HEAD_DIM), D ** -0.5, 0.09375, ((1, 8),))
    w_decay = gaussian(splits[6], (D, HEADS), D ** -0.5, 0.09375)
    w_beta = gaussian(splits[7], (D, HEADS), D ** -0.5, 0.09375)
    decay_rate = jnp.clip(jnp.exp(math.log(3.0) - 4.6051702 * jax.random.uniform(splits[8], (HEADS,), jnp.float32) ** levels(splits[8], (HEADS,), ((0, 8),), -0.2, 0.2)), 0.03, 3.0)
    decay_bias = jnp.clip(jax.random.uniform(splits[9], (HEADS,), jnp.float32, -1.0, 1.0) * levels(splits[9], (HEADS,), ((0, 8),), -0.4, 0.0), -1.0, 1.0)
    mix_gain = jnp.clip(1.0 + 0.18 * jax.random.normal(splits[10], (D,), jnp.float32), 0.1, 1.9)
    out_gain = jnp.clip(1.0 + 0.18 * jax.random.normal(splits[11], (HEAD_DIM,), jnp.float32), 0.1, 1.9)
    w_out = gaussian(splits[12], (HEADS * HEAD_DIM, D), (HEADS * HEAD_DIM) ** -0.5, 0.125, ((0, 8),))
    ffn_gain = jnp.clip(1.0 + 0.18 * jax.random.normal(splits[13], (D,), jnp.float32), 0.1, 1.9)
    w_up = gaussian(splits[14], (D, FF), D ** -0.5, 0.09375, ((0, 8), (1, 4)))
    w_down = gaussian(splits[15], (FF, D), FF ** -0.5, 0.046875, ((0, 4), (1, 8)))
    return {"tokens": tokens, "state": state, "w_query": w_query, "w_key": w_key, "w_value": w_value, "w_gate": w_gate, "w_decay": w_decay, "w_beta": w_beta, "decay_rate": decay_rate, "decay_bias": decay_bias, "mix_gain": mix_gain, "out_gain": out_gain, "w_out": w_out, "ffn_gain": ffn_gain, "w_up": w_up, "w_down": w_down}


EPS = 1e-06

def unit_norm(vector):
    return vector * lax.rsqrt(lax.optimization_barrier(jnp.sum(vector * vector, axis=-1, keepdims=True)) + EPS)

def reference(tokens, state, w_query, w_key, w_value, w_gate, w_decay, w_beta, decay_rate, decay_bias, mix_gain, out_gain, w_out, ffn_gain, w_up, w_down):
    rows = tokens.shape[0]
    tok_f = tokens.astype(jnp.float32)
    normed = (tok_f * lax.rsqrt(lax.optimization_barrier(jnp.mean(tok_f * tok_f, axis=-1, keepdims=True)) + EPS) * mix_gain).astype(jnp.bfloat16)
    query = jnp.dot(normed, w_query, preferred_element_type=jnp.float32).reshape(rows, HEADS, HEAD_DIM)
    key_proj = jnp.dot(normed, w_key, preferred_element_type=jnp.float32).reshape(rows, HEADS, HEAD_DIM)
    value = jnp.dot(normed, w_value, preferred_element_type=jnp.float32).reshape(rows, HEADS, HEAD_DIM)
    gate = jnp.dot(normed, w_gate, preferred_element_type=jnp.float32).reshape(rows, HEADS, HEAD_DIM)
    query = unit_norm(query) * HEAD_DIM ** (-0.5)
    key_proj = unit_norm(key_proj)
    pre_decay = jnp.dot(normed, w_decay, preferred_element_type=jnp.float32)
    decay = jnp.exp(-decay_rate * jax.nn.softplus(pre_decay + decay_bias))
    strength = jax.nn.sigmoid(jnp.dot(normed, w_beta, preferred_element_type=jnp.float32))
    matrix = state.reshape(rows, HEADS, HEAD_DIM, HEAD_DIM) * decay[:, :, None, None]
    recalled = jnp.einsum('bhk,bhkv->bhv', key_proj, matrix, precision=lax.Precision.HIGHEST)
    delta = (value - recalled) * strength[:, :, None]
    matrix = matrix + key_proj[:, :, :, None] * delta[:, :, None, :]
    head_out = jnp.einsum('bhk,bhkv->bhv', query, matrix, precision=lax.Precision.HIGHEST)
    head_out = head_out * lax.rsqrt(lax.optimization_barrier(jnp.mean(head_out * head_out, axis=-1, keepdims=True)) + EPS) * out_gain * jax.nn.silu(gate)
    head_out = head_out.reshape(rows, HEADS * HEAD_DIM).astype(jnp.bfloat16)
    resid = tok_f + jnp.dot(head_out, w_out, preferred_element_type=jnp.float32)
    ffn_in = (resid * lax.rsqrt(lax.optimization_barrier(jnp.mean(resid * resid, axis=-1, keepdims=True)) + EPS) * ffn_gain).astype(jnp.bfloat16)
    hidden = jnp.square(jax.nn.relu(jnp.dot(ffn_in, w_up, preferred_element_type=jnp.float32))).astype(jnp.bfloat16)
    mixed = (resid + jnp.dot(hidden, w_down, preferred_element_type=jnp.float32)).astype(jnp.bfloat16)
    return (mixed, matrix.reshape(rows, HEADS, HEAD_DIM * HEAD_DIM))
```

```python
import functools

import jax
import jax.numpy as jnp
from jax import lax
from jax.experimental import pallas as pl
from jax.experimental.pallas import tpu as pltpu
from jax.sharding import PartitionSpec as P

HEAD_DIM = 64


EPS = 1e-06


def unit_norm(vector):
    return vector * lax.rsqrt(jnp.sum(vector * vector, axis=-1, keepdims=True) + EPS)


MESH = pl.DeviceIdType.MESH
VMEM = pltpu.VMEM
CORES = 2


def remote(src, dst, send, recv, where):
    return pltpu.make_async_remote_copy(
        src_ref=src, dst_ref=dst, send_sem=send, recv_sem=recv, device_id=where, device_id_type=MESH
    )


def place(chips):
    me = lax.axis_index("tp")
    return lax.div(me, CORES), lax.rem(me, CORES)


def columns(block, width):
    return pl.ds(pl.multiple_of(block * width, 128), width)


def gather_kernel(chips, x_ref, o_ref, own_sem, send, recv, pass_send, pass_recv):
    chip, core = place(chips)
    width = x_ref.shape[1]
    partner = {"tp": chip * CORES + 1 - core}

    def peer(step):
        return {"tp": lax.rem(chip + step, chips) * CORES + core}

    barrier = pltpu.get_barrier_semaphore()
    pl.semaphore_signal(barrier, inc=1, device_id=partner, device_id_type=MESH)
    for step in range(1, chips):
        pl.semaphore_signal(barrier, inc=1, device_id=peer(step), device_id_type=MESH)
    pl.semaphore_wait(barrier, chips)

    mine = columns(chip * CORES + core, width)
    copies = []
    for step in range(1, chips):
        copies.append(remote(x_ref, o_ref.at[:, mine], send.at[step], recv.at[step], peer(step)))
        copies[-1].start()
    near = remote(x_ref, o_ref.at[:, mine], send.at[0], recv.at[0], partner)
    near.start()
    keep = pltpu.make_async_copy(x_ref, o_ref.at[:, mine], own_sem)
    keep.start()
    passed = []
    for step in range(1, chips):
        copies[step - 1].wait_recv()
        block = lax.rem(chip + chips - step, chips) * CORES + core
        there = o_ref.at[:, columns(block, width)]
        passed.append(remote(there, there, pass_send.at[step], pass_recv.at[step], partner))
        passed[-1].start()
    near.wait()
    keep.wait()
    for copy in passed:
        copy.wait()
    for copy in copies:
        copy.wait_send()


def gather_tp(tokens, chips):
    rows, width = tokens.shape
    return pl.pallas_call(
        functools.partial(gather_kernel, chips),
        out_shape=jax.ShapeDtypeStruct((rows, width * chips * CORES), tokens.dtype),
        in_specs=[pl.BlockSpec(memory_space=VMEM)],
        out_specs=pl.BlockSpec(memory_space=VMEM),
        scratch_shapes=[pltpu.SemaphoreType.DMA] + [pltpu.SemaphoreType.DMA((chips,))] * 4,
        compiler_params=pltpu.CompilerParams(collective_id=0, has_side_effects=True),
        name="gather_tp",
    )(tokens)


def mixer_kernel(
    chips, groups, part_ref, tok_ref, gain_ref, up_ref, down_hbm, o_ref,
    down_ref, pair_in, pair_sum, chip_in, resid_ref, y_ref, sq_ref,
    up_out, up_in, up_sum, up_far, up_acc, h_ref, acc_ref, d_out, d_in,
    load_sem, s_pair, r_pair, s_chip, r_chip, s_y, r_y, s_sq, r_sq,
    s_up, r_up, s_far, r_far, s_h, r_h, s_pass, r_pass, s_d, r_d,
):
    chip, core = place(chips)
    me = chip * CORES + core
    group = lax.axis_index("kv")
    ranks = chips * CORES
    rows, width = tok_ref.shape
    hid = up_ref.shape[1] // ranks
    partner = {"tp": chip * CORES + 1 - core}
    f32, bf16 = jnp.float32, jnp.bfloat16

    def ahead(step):
        return lax.rem(chip + step, chips)

    def behind(step):
        return lax.rem(chip + chips - step, chips)

    def peer(step):
        return {"tp": ahead(step) * CORES + core}

    def rank_peer(step):
        return {"tp": lax.rem(me + step, ranks)}

    def group_peer(step):
        return {"kv": lax.rem(group + step, groups)}

    barrier = pltpu.get_barrier_semaphore()
    for step in range(1, ranks):
        pl.semaphore_signal(barrier, inc=1, device_id=rank_peer(step), device_id_type=MESH)
    for step in range(1, groups):
        pl.semaphore_signal(barrier, inc=1, device_id=group_peer(step), device_id_type=MESH)
    load = pltpu.make_async_copy(down_hbm, down_ref, load_sem)
    load.start()
    pl.semaphore_wait(barrier, ranks + groups - 2)

    order = list(range(1, chips)) + [0]
    pair = {}
    for step in order:
        there = part_ref.at[:, columns(ahead(step) * CORES + 1 - core, width)]
        pair[step] = remote(there, pair_in.at[step], s_pair.at[step], r_pair.at[step], partner)
        pair[step].start()
    far = {}
    for step in order:
        pair[step].wait_recv()
        both = part_ref[:, columns(ahead(step) * CORES + core, width)].astype(f32) + pair_in[
            step
        ].astype(f32)
        if step:
            pair_sum[step] = both.astype(bf16)
            far[step] = remote(
                pair_sum.at[step], chip_in.at[step], s_chip.at[step], r_chip.at[step], peer(step)
            )
            far[step].start()
    resid = tok_ref[...].astype(f32) + both
    for step in range(1, chips):
        far[step].wait_recv()
        resid = resid + chip_in[step].astype(f32)
    resid_ref[...] = resid
    y_ref[0] = (resid * gain_ref[...]).astype(bf16)
    spread = {}
    for step in range(1, groups):
        spread[step] = remote(
            y_ref.at[0], y_ref.at[step], s_y.at[step], r_y.at[step], group_peer(step)
        )
        spread[step].start()
    sq_ref[0] = lax.dot_general(
        jnp.ones((8, width), f32),
        resid * resid,
        (((1,), (1,)), ((), ())),
        precision=lax.Precision.HIGHEST,
        preferred_element_type=f32,
    )
    squares = {}
    for step in range(1, ranks):
        squares[step] = remote(
            sq_ref.at[0], sq_ref.at[step], s_sq.at[step], r_sq.at[step], rank_peer(step)
        )
        squares[step].start()
    for step in range(1, groups):
        spread[step].wait_recv()

    all_rows = groups * rows

    def up_block(block):
        return jnp.dot(
            y_ref[...].reshape(all_rows, width),
            up_ref[:, columns(block, hid)],
            preferred_element_type=f32,
        )

    def up_pair(step):
        return remote(up_out.at[step], up_in.at[step], s_up.at[step], r_up.at[step], partner)

    def up_chip(step):
        return remote(up_sum.at[step], up_far.at[step], s_far.at[step], r_far.at[step], peer(step))

    @pl.loop(0, chips)
    def _(index):
        step = lax.rem(index + 1, chips)
        up_out[step] = up_block(ahead(step) * CORES + 1 - core).astype(bf16)
        up_pair(step).start()

    @pl.loop(1, chips)
    def _(step):
        both = up_block(ahead(step) * CORES + core)
        up_pair(step).wait_recv()
        up_sum[step] = (both + up_in[step].astype(f32)).astype(bf16)
        up_chip(step).start()

    up_acc[...] = up_block(me)
    up_pair(0).wait_recv()
    up_acc[...] += up_in[0].astype(f32)

    @pl.loop(1, chips)
    def _(step):
        up_chip(step).wait_recv()
        up_acc[...] += up_far[step].astype(f32)

    h_ref[0] = jnp.square(jnp.maximum(up_acc[...], 0.0)).astype(bf16)

    def h_chip(step):
        return remote(h_ref.at[0], h_ref.at[step], s_h.at[step], r_h.at[step], peer(step))

    def h_pass(step):
        return remote(
            h_ref.at[step], h_ref.at[chips + step], s_pass.at[step], r_pass.at[step], partner
        )

    @pl.loop(1, chips)
    def _(step):
        h_chip(step).start()

    h_pass(0).start()
    load.wait()

    def down_block(slot, block):
        return jnp.dot(
            h_ref[slot],
            down_ref[pl.ds(pl.multiple_of(block * hid, 128), hid), :],
            preferred_element_type=f32,
        )

    acc_ref[...] = down_block(0, me)
    h_pass(0).wait_recv()
    acc_ref[...] += down_block(chips, chip * CORES + 1 - core)

    @pl.loop(1, chips)
    def _(step):
        h_chip(step).wait_recv()
        h_pass(step).start()
        acc_ref[...] += down_block(step, behind(step) * CORES + core)
        h_pass(step).wait_recv()
        acc_ref[...] += down_block(chips + step, behind(step) * CORES + 1 - core)

    back = {}
    for step in range(1, groups):
        d_out[step] = acc_ref[step * rows : (step + 1) * rows, :].astype(bf16)
        back[step] = remote(
            d_out.at[step], d_in.at[step], s_d.at[step], r_d.at[step], group_peer(groups - step)
        )
        back[step].start()
    for step in range(1, ranks):
        squares[step].wait_recv()
    total = sq_ref[0]
    for step in range(1, ranks):
        total = total + sq_ref[step]
    spots = lax.dot_general(
        total,
        jnp.full((8, width), 0.125, f32),
        (((0,), (0,)), ((), ())),
        precision=lax.Precision.HIGHEST,
        preferred_element_type=f32,
    )
    scale = lax.rsqrt(spots * (1.0 / (width * ranks)) + EPS)
    mixed = acc_ref[0:rows, :]
    for step in range(1, groups):
        back[step].wait_recv()
        mixed = mixed + d_in[step].astype(f32)
    o_ref[...] = (resid_ref[...] + scale * scale * mixed).astype(bf16)

    for copies in (pair, far, spread, squares, back):
        for copy in copies.values():
            copy.wait_send()
    h_pass(0).wait_send()
    up_pair(0).wait_send()

    @pl.loop(1, chips)
    def _(step):
        up_pair(step).wait_send()
        up_chip(step).wait_send()
        h_chip(step).wait_send()
        h_pass(step).wait_send()


def channel_mixer(partial_value, tokens, gain_share, w_up, w_down, chips, groups):
    rows, width = tokens.shape
    ranks = chips * CORES
    hid = w_up.shape[1] // ranks
    all_rows = groups * rows
    bf16, f32 = jnp.bfloat16, jnp.float32
    dma = pltpu.SemaphoreType.DMA
    spec = pl.BlockSpec(memory_space=VMEM)
    return pl.pallas_call(
        functools.partial(mixer_kernel, chips, groups),
        out_shape=jax.ShapeDtypeStruct((rows, width), bf16),
        in_specs=[spec] * 4 + [pl.BlockSpec(memory_space=pl.ANY)],
        out_specs=spec,
        scratch_shapes=[
            VMEM(w_down.shape, bf16),
            VMEM((chips, rows, width), bf16),
            VMEM((chips, rows, width), bf16),
            VMEM((chips, rows, width), bf16),
            VMEM((rows, width), f32),
            VMEM((groups, rows, width), bf16),
            VMEM((ranks, 8, rows), f32),
            VMEM((chips, all_rows, hid), bf16),
            VMEM((chips, all_rows, hid), bf16),
            VMEM((chips, all_rows, hid), bf16),
            VMEM((chips, all_rows, hid), bf16),
            VMEM((all_rows, hid), f32),
            VMEM((ranks, all_rows, hid), bf16),
            VMEM((all_rows, width), f32),
            VMEM((groups, rows, width), bf16),
            VMEM((groups, rows, width), bf16),
            dma,
        ]
        + [dma((chips,))] * 4
        + [dma((groups,))] * 2
        + [dma((ranks,))] * 2
        + [dma((chips,))] * 8
        + [dma((groups,))] * 2,
        compiler_params=pltpu.CompilerParams(
            collective_id=1, has_side_effects=True, vmem_limit_bytes=48 * 1024 * 1024
        ),
        name="channel_mixer",
    )(partial_value, tokens, gain_share, w_up, w_down)


def local(
    chips,
    groups,
    tokens,
    state,
    w_query,
    w_key,
    w_value,
    w_gate,
    w_decay,
    w_beta,
    decay_rate,
    decay_bias,
    mix_gain,
    out_gain,
    w_out,
    ffn_gain,
    w_up,
    w_down,
):
    rows = tokens.shape[0]
    width_share = tokens.shape[1]
    head_count = w_query.shape[1] // HEAD_DIM
    full_rows = gather_tp(tokens, chips)
    full_f = full_rows.astype(jnp.float32)
    normed = (
        full_f * lax.rsqrt(jnp.mean(full_f * full_f, axis=-1, keepdims=True) + EPS) * mix_gain
    ).astype(jnp.bfloat16)
    query = jnp.dot(normed, w_query, preferred_element_type=jnp.float32).reshape(
        rows, head_count, HEAD_DIM
    )
    key_proj = jnp.dot(normed, w_key, preferred_element_type=jnp.float32).reshape(
        rows, head_count, HEAD_DIM
    )
    value = jnp.dot(normed, w_value, preferred_element_type=jnp.float32).reshape(
        rows, head_count, HEAD_DIM
    )
    gate = jnp.dot(normed, w_gate, preferred_element_type=jnp.float32).reshape(
        rows, head_count, HEAD_DIM
    )
    query = unit_norm(query) * HEAD_DIM ** (-0.5)
    key_proj = unit_norm(key_proj)
    head_start = lax.axis_index("tp") * head_count
    decay_cols = lax.dynamic_slice_in_dim(w_decay, head_start, head_count, 1)
    beta_cols = lax.dynamic_slice_in_dim(w_beta, head_start, head_count, 1)
    pre_decay = jnp.dot(normed, decay_cols, preferred_element_type=jnp.float32)
    decay = jnp.exp(-decay_rate * jax.nn.softplus(pre_decay + decay_bias))
    strength = jax.nn.sigmoid(jnp.dot(normed, beta_cols, preferred_element_type=jnp.float32))
    matrix = state.reshape(rows, head_count, HEAD_DIM, HEAD_DIM) * decay[:, :, None, None]
    recalled = jnp.einsum("bhk,bhkv->bhv", key_proj, matrix, precision=lax.Precision.HIGHEST)
    delta = (value - recalled) * strength[:, :, None]
    matrix = matrix + key_proj[:, :, :, None] * delta[:, :, None, :]
    head_out = jnp.einsum("bhk,bhkv->bhv", query, matrix, precision=lax.Precision.HIGHEST)
    head_out = (
        head_out
        * lax.rsqrt(jnp.mean(head_out * head_out, axis=-1, keepdims=True) + EPS)
        * out_gain
        * jax.nn.silu(gate)
    )
    head_out = head_out.reshape(rows, head_count * HEAD_DIM).astype(jnp.bfloat16)
    partial_value = jnp.dot(head_out, w_out, preferred_element_type=jnp.float32)
    feature_start = lax.axis_index("tp") * width_share
    gain_share = lax.dynamic_slice_in_dim(ffn_gain, feature_start, width_share, 0)
    mixed = channel_mixer(
        partial_value.astype(jnp.bfloat16),
        tokens,
        gain_share[None, :],
        w_up,
        w_down,
        chips,
        groups,
    )
    return (mixed, matrix.reshape(rows, head_count, HEAD_DIM * HEAD_DIM))


def solution(mesh):
    in_specs = (
        P("kv", "tp"),
        P("kv", "tp", None),
        P(None, "tp"),
        P(None, "tp"),
        P(None, "tp"),
        P(None, "tp"),
        P(),
        P(),
        P("tp"),
        P("tp"),
        P(),
        P(),
        P("tp", None),
        P(),
        P("tp", "kv"),
        P("kv", "tp"),
    )
    out_specs = (P("kv", "tp"), P("kv", "tp", None))
    body = functools.partial(local, mesh.shape["tp"] // CORES, mesh.shape["kv"])
    return jax.shard_map(body, mesh=mesh, in_specs=in_specs, out_specs=out_specs, check_vma=False)
```

```python
import functools

import jax
import jax.numpy as jnp
from jax import lax
from jax.experimental import pallas as pl
from jax.experimental.pallas import tpu as pltpu
from jax.sharding import PartitionSpec as P

HEAD_DIM = 64


EPS = 1e-06


def unit_norm(vector):
    return vector * lax.rsqrt(jnp.sum(vector * vector, axis=-1, keepdims=True) + EPS)


MESH = pl.DeviceIdType.MESH
VMEM = pltpu.VMEM
CORES = 2


def remote(src, dst, send, recv, where):
    return pltpu.make_async_remote_copy(
        src_ref=src, dst_ref=dst, send_sem=send, recv_sem=recv, device_id=where, device_id_type=MESH
    )


def place(chips):
    me = lax.axis_index("tp")
    return lax.div(me, CORES), lax.rem(me, CORES)


def columns(block, width):
    return pl.ds(pl.multiple_of(block * width, 128), width)


def gather_kernel(chips, x_ref, o_ref, own_sem, send, recv, pass_send, pass_recv):
    chip, core = place(chips)
    width = x_ref.shape[1]
    partner = {"tp": chip * CORES + 1 - core}

    def peer(step):
        return {"tp": lax.rem(chip + step, chips) * CORES + core}

    barrier = pltpu.get_barrier_semaphore()
    pl.semaphore_signal(barrier, inc=1, device_id=partner, device_id_type=MESH)
    for step in range(1, chips):
        pl.semaphore_signal(barrier, inc=1, device_id=peer(step), device_id_type=MESH)
    pl.semaphore_wait(barrier, chips)

    mine = columns(chip * CORES + core, width)
    copies = []
    for step in range(1, chips):
        copies.append(remote(x_ref, o_ref.at[:, mine], send.at[step], recv.at[step], peer(step)))
        copies[-1].start()
    near = remote(x_ref, o_ref.at[:, mine], send.at[0], recv.at[0], partner)
    near.start()
    keep = pltpu.make_async_copy(x_ref, o_ref.at[:, mine], own_sem)
    keep.start()
    passed = []
    for step in range(1, chips):
        copies[step - 1].wait_recv()
        block = lax.rem(chip + chips - step, chips) * CORES + core
        there = o_ref.at[:, columns(block, width)]
        passed.append(remote(there, there, pass_send.at[step], pass_recv.at[step], partner))
        passed[-1].start()
    near.wait()
    keep.wait()
    for copy in passed:
        copy.wait()
    for copy in copies:
        copy.wait_send()


def gather_tp(tokens, chips):
    rows, width = tokens.shape
    return pl.pallas_call(
        functools.partial(gather_kernel, chips),
        out_shape=jax.ShapeDtypeStruct((rows, width * chips * CORES), tokens.dtype),
        in_specs=[pl.BlockSpec(memory_space=VMEM)],
        out_specs=pl.BlockSpec(memory_space=VMEM),
        scratch_shapes=[pltpu.SemaphoreType.DMA] + [pltpu.SemaphoreType.DMA((chips,))] * 4,
        compiler_params=pltpu.CompilerParams(collective_id=0, has_side_effects=True),
        name="gather_tp",
    )(tokens)


def mixer_kernel(
    chips, groups, part_ref, tok_ref, gain_ref, up_ref, down_hbm, o_ref,
    down_ref, pair_in, pair_sum, chip_in, resid_ref, y_ref, sq_ref,
    up_out, up_in, up_sum, up_far, up_acc, h_ref, acc_ref, d_out, d_in,
    load_sem, s_pair, r_pair, s_chip, r_chip, s_y, r_y, s_sq, r_sq,
    s_up, r_up, s_far, r_far, s_h, r_h, s_pass, r_pass, s_d, r_d,
):
    chip, core = place(chips)
    me = chip * CORES + core
    group = lax.axis_index("kv")
    ranks = chips * CORES
    rows, width = tok_ref.shape
    hid = up_ref.shape[1] // ranks
    partner = {"tp": chip * CORES + 1 - core}
    f32, bf16 = jnp.float32, jnp.bfloat16

    def ahead(step):
        return lax.rem(chip + step, chips)

    def behind(step):
        return lax.rem(chip + chips - step, chips)

    def peer(step):
        return {"tp": ahead(step) * CORES + core}

    def rank_peer(step):
        return {"tp": lax.rem(me + step, ranks)}

    def group_peer(step):
        return {"kv": lax.rem(group + step, groups)}

    barrier = pltpu.get_barrier_semaphore()
    for step in range(1, ranks):
        pl.semaphore_signal(barrier, inc=1, device_id=rank_peer(step), device_id_type=MESH)
    for step in range(1, groups):
        pl.semaphore_signal(barrier, inc=1, device_id=group_peer(step), device_id_type=MESH)
    load = pltpu.make_async_copy(down_hbm, down_ref, load_sem)
    load.start()
    pl.semaphore_wait(barrier, ranks + groups - 2)

    order = list(range(1, chips)) + [0]
    pair = {}
    for step in order:
        there = part_ref.at[:, columns(ahead(step) * CORES + 1 - core, width)]
        pair[step] = remote(there, pair_in.at[step], s_pair.at[step], r_pair.at[step], partner)
        pair[step].start()
    far = {}
    for step in order:
        pair[step].wait_recv()
        both = part_ref[:, columns(ahead(step) * CORES + core, width)].astype(f32) + pair_in[
            step
        ].astype(f32)
        if step:
            pair_sum[step] = both.astype(bf16)
            far[step] = remote(
                pair_sum.at[step], chip_in.at[step], s_chip.at[step], r_chip.at[step], peer(step)
            )
            far[step].start()
    resid = tok_ref[...].astype(f32) + both
    for step in range(1, chips):
        far[step].wait_recv()
        resid = resid + chip_in[step].astype(f32)
    resid_ref[...] = resid
    y_ref[0] = (resid * gain_ref[...]).astype(bf16)
    spread = {}
    for step in range(1, groups):
        spread[step] = remote(
            y_ref.at[0], y_ref.at[step], s_y.at[step], r_y.at[step], group_peer(step)
        )
        spread[step].start()
    sq_ref[0] = lax.dot_general(
        jnp.ones((8, width), f32),
        resid * resid,
        (((1,), (1,)), ((), ())),
        precision=lax.Precision.HIGHEST,
        preferred_element_type=f32,
    )
    squares = {}
    for step in range(1, ranks):
        squares[step] = remote(
            sq_ref.at[0], sq_ref.at[step], s_sq.at[step], r_sq.at[step], rank_peer(step)
        )
        squares[step].start()
    for step in range(1, groups):
        spread[step].wait_recv()

    all_rows = groups * rows

    def up_block(block):
        return jnp.dot(
            y_ref[...].reshape(all_rows, width),
            up_ref[:, columns(block, hid)],
            preferred_element_type=f32,
        )

    def up_pair(step):
        return remote(up_out.at[step], up_in.at[step], s_up.at[step], r_up.at[step], partner)

    def up_chip(step):
        return remote(up_sum.at[step], up_far.at[step], s_far.at[step], r_far.at[step], peer(step))

    @pl.loop(0, chips)
    def _(index):
        step = lax.rem(index + 1, chips)
        up_out[step] = up_block(ahead(step) * CORES + 1 - core).astype(bf16)
        up_pair(step).start()

    @pl.loop(1, chips)
    def _(step):
        both = up_block(ahead(step) * CORES + core)
        up_pair(step).wait_recv()
        up_sum[step] = (both + up_in[step].astype(f32)).astype(bf16)
        up_chip(step).start()

    up_acc[...] = up_block(me)
    up_pair(0).wait_recv()
    up_acc[...] += up_in[0].astype(f32)

    @pl.loop(1, chips)
    def _(step):
        up_chip(step).wait_recv()
        up_acc[...] += up_far[step].astype(f32)

    h_ref[0] = jnp.square(jnp.maximum(up_acc[...], 0.0)).astype(bf16)

    def h_chip(step):
        return remote(h_ref.at[0], h_ref.at[step], s_h.at[step], r_h.at[step], peer(step))

    def h_pass(step):
        return remote(
            h_ref.at[step], h_ref.at[chips + step], s_pass.at[step], r_pass.at[step], partner
        )

    @pl.loop(1, chips)
    def _(step):
        h_chip(step).start()

    h_pass(0).start()
    load.wait()

    def down_block(slot, block):
        return jnp.dot(
            h_ref[slot],
            down_ref[pl.ds(pl.multiple_of(block * hid, 128), hid), :],
            preferred_element_type=f32,
        )

    acc_ref[...] = down_block(0, me)
    h_pass(0).wait_recv()
    acc_ref[...] += down_block(chips, chip * CORES + 1 - core)

    @pl.loop(1, chips)
    def _(step):
        h_chip(step).wait_recv()
        h_pass(step).start()
        acc_ref[...] += down_block(step, behind(step) * CORES + core)
        h_pass(step).wait_recv()
        acc_ref[...] += down_block(chips + step, behind(step) * CORES + 1 - core)

    back = {}
    for step in range(1, groups):
        d_out[step] = acc_ref[step * rows : (step + 1) * rows, :].astype(bf16)
        back[step] = remote(
            d_out.at[step], d_in.at[step], s_d.at[step], r_d.at[step], group_peer(groups - step)
        )
        back[step].start()
    for step in range(1, ranks):
        squares[step].wait_recv()
    total = sq_ref[0]
    for step in range(1, ranks):
        total = total + sq_ref[step]
    spots = lax.dot_general(
        total,
        jnp.full((8, width), 0.125, f32),
        (((0,), (0,)), ((), ())),
        precision=lax.Precision.HIGHEST,
        preferred_element_type=f32,
    )
    scale = lax.rsqrt(spots * (1.0 / (width * ranks)) + EPS)
    mixed = acc_ref[0:rows, :]
    for step in range(1, groups):
        back[step].wait_recv()
        mixed = mixed + d_in[step].astype(f32)
    o_ref[...] = (resid_ref[...] + scale * scale * mixed).astype(bf16)

    for copies in (pair, far, spread, squares, back):
        for copy in copies.values():
            copy.wait_send()
    h_pass(0).wait_send()
    up_pair(0).wait_send()

    @pl.loop(1, chips)
    def _(step):
        up_pair(step).wait_send()
        up_chip(step).wait_send()
        h_chip(step).wait_send()
        h_pass(step).wait_send()


def channel_mixer(partial_value, tokens, gain_share, w_up, w_down, chips, groups):
    rows, width = tokens.shape
    ranks = chips * CORES
    hid = w_up.shape[1] // ranks
    all_rows = groups * rows
    bf16, f32 = jnp.bfloat16, jnp.float32
    dma = pltpu.SemaphoreType.DMA
    spec = pl.BlockSpec(memory_space=VMEM)
    return pl.pallas_call(
        functools.partial(mixer_kernel, chips, groups),
        out_shape=jax.ShapeDtypeStruct((rows, width), bf16),
        in_specs=[spec] * 4 + [pl.BlockSpec(memory_space=pl.ANY)],
        out_specs=spec,
        scratch_shapes=[
            VMEM(w_down.shape, bf16),
            VMEM((chips, rows, width), bf16),
            VMEM((chips, rows, width), bf16),
            VMEM((chips, rows, width), bf16),
            VMEM((rows, width), f32),
            VMEM((groups, rows, width), bf16),
            VMEM((ranks, 8, rows), f32),
            VMEM((chips, all_rows, hid), bf16),
            VMEM((chips, all_rows, hid), bf16),
            VMEM((chips, all_rows, hid), bf16),
            VMEM((chips, all_rows, hid), bf16),
            VMEM((all_rows, hid), f32),
            VMEM((ranks, all_rows, hid), bf16),
            VMEM((all_rows, width), f32),
            VMEM((groups, rows, width), bf16),
            VMEM((groups, rows, width), bf16),
            dma,
        ]
        + [dma((chips,))] * 4
        + [dma((groups,))] * 2
        + [dma((ranks,))] * 2
        + [dma((chips,))] * 8
        + [dma((groups,))] * 2,
        compiler_params=pltpu.CompilerParams(
            collective_id=1, has_side_effects=True, vmem_limit_bytes=48 * 1024 * 1024
        ),
        name="channel_mixer",
    )(partial_value, tokens, gain_share, w_up, w_down)


def doubled(x):
    return jnp.concatenate([x, x], axis=-1)


def state_kernel(
    heads, proj_ref, rates_ref, gain_ref, state_ref, new_ref, out_ref,
    spread_ref, wide_ref, val_ref, row_ref, head_ref,
):
    f32, bf16 = jnp.float32, jnp.bfloat16
    lanes = 2 * HEAD_DIM
    count = out_ref.shape[0]
    full = state_ref.shape[2]
    pack = 8 // heads

    @pl.when(pl.program_id(0) == 0)
    def _():
        feature = lax.broadcasted_iota(jnp.int32, spread_ref.shape, 0)
        lane = lax.broadcasted_iota(jnp.int32, spread_ref.shape, 1)
        hit = lax.rem(feature, HEAD_DIM) == lax.div(lane, HEAD_DIM)
        spread_ref[...] = jnp.where(hit, 1.0, 0.0).astype(bf16)

    query = unit_norm(proj_ref[0]) * HEAD_DIM ** (-0.5)
    key_proj = unit_norm(proj_ref[1])
    match = jnp.sum(query * key_proj, axis=-1, keepdims=True)
    both = doubled(jnp.concatenate([key_proj, query], axis=0))
    high = both.astype(bf16).astype(f32)
    rest = both - high
    middle = rest.astype(bf16).astype(f32)
    low = rest - middle
    first = lax.broadcasted_iota(jnp.int32, both.shape, 1) < HEAD_DIM
    parts = jnp.concatenate(
        [jnp.where(first, high, middle), jnp.where(first, low, 0.0)], axis=-1
    ).astype(bf16)
    wide_ref[...] = jnp.dot(parts, spread_ref[...], preferred_element_type=f32)
    val_ref[...] = doubled(proj_ref[2])
    row_ref[0] = jnp.broadcast_to(rates_ref[:, 0:1], (count, lanes))
    row_ref[1] = jnp.broadcast_to(rates_ref[:, 1:2], (count, lanes))
    row_ref[2] = jnp.broadcast_to(match, (count, lanes))

    @pl.loop(0, count // 8)
    def _(index):
        here = pl.ds(pl.multiple_of(index * 8, 8), 8)
        there = pl.ds(pl.multiple_of(index * 8 + count, 8), 8)

        def state_at(at):
            return jnp.concatenate(
                [state_ref[index * pack + i, :, at] for i in range(pack)], axis=0
            )

        by_key = jnp.zeros((8, lanes), f32)
        by_query = jnp.zeros((8, lanes), f32)
        for start in range(0, full, lanes):
            at = slice(start, start + lanes)
            now = state_at(at)
            by_key = by_key + now * wide_ref[here, at]
            by_query = by_query + now * wide_ref[there, at]
        by_key = by_key + pltpu.roll(by_key, HEAD_DIM, 1)
        by_query = by_query + pltpu.roll(by_query, HEAD_DIM, 1)
        decay = row_ref[0, here, :]
        delta = (val_ref[here, :] - decay * by_key) * row_ref[1, here, :]
        head_ref[here, :] = decay * by_query + row_ref[2, here, :] * delta
        for start in range(0, full, lanes):
            at = slice(start, start + lanes)
            new = decay * state_at(at) + wide_ref[here, at] * delta
            for i in range(pack):
                new_ref[index * pack + i, :, at] = new[i * heads : (i + 1) * heads]

    head_out = head_ref[:, 0:HEAD_DIM]
    gate = proj_ref[3]
    out_ref[...] = (
        head_out
        * lax.rsqrt(jnp.mean(head_out * head_out, axis=-1, keepdims=True) + EPS)
        * gain_ref[...]
        * (gate * jax.nn.sigmoid(gate))
    ).astype(bf16)


def update_state(proj, rates, out_gain, state):
    rows, heads, full = state.shape
    block = rows // 3
    count = block * heads
    f32, bf16 = jnp.float32, jnp.bfloat16
    return pl.pallas_call(
        functools.partial(state_kernel, heads),
        grid=(rows // block,),
        out_shape=(
            jax.ShapeDtypeStruct(state.shape, f32),
            jax.ShapeDtypeStruct((rows * heads, HEAD_DIM), bf16),
        ),
        in_specs=[
            pl.BlockSpec((4, count, HEAD_DIM), lambda i: (0, i, 0)),
            pl.BlockSpec((count, 2), lambda i: (i, 0)),
            pl.BlockSpec((1, HEAD_DIM), lambda i: (0, 0)),
            pl.BlockSpec((block, heads, full), lambda i: (i, 0, 0)),
        ],
        out_specs=(
            pl.BlockSpec((block, heads, full), lambda i: (i, 0, 0)),
            pl.BlockSpec((count, HEAD_DIM), lambda i: (i, 0)),
        ),
        scratch_shapes=[
            VMEM((4 * HEAD_DIM, full), bf16),
            VMEM((2 * count, full), f32),
            VMEM((count, 2 * HEAD_DIM), f32),
            VMEM((3, count, 2 * HEAD_DIM), f32),
            VMEM((count, 2 * HEAD_DIM), f32),
        ],
        compiler_params=pltpu.CompilerParams(vmem_limit_bytes=32 * 1024 * 1024),
        name="update_state",
    )(proj, rates, out_gain, state)


def local(
    chips,
    groups,
    tokens,
    state,
    w_query,
    w_key,
    w_value,
    w_gate,
    w_decay,
    w_beta,
    decay_rate,
    decay_bias,
    mix_gain,
    out_gain,
    w_out,
    ffn_gain,
    w_up,
    w_down,
):
    rows = tokens.shape[0]
    width_share = tokens.shape[1]
    head_count = w_query.shape[1] // HEAD_DIM
    full_rows = gather_tp(tokens, chips)
    full_f = full_rows.astype(jnp.float32)
    normed = (
        full_f * lax.rsqrt(jnp.mean(full_f * full_f, axis=-1, keepdims=True) + EPS) * mix_gain
    ).astype(jnp.bfloat16)
    proj = jnp.stack(
        [
            jnp.dot(normed, w, preferred_element_type=jnp.float32)
            for w in (w_query, w_key, w_value, w_gate)
        ]
    ).reshape(4, rows * head_count, HEAD_DIM)
    head_start = lax.axis_index("tp") * head_count
    decay_cols = lax.dynamic_slice_in_dim(w_decay, head_start, head_count, 1)
    beta_cols = lax.dynamic_slice_in_dim(w_beta, head_start, head_count, 1)
    pre_decay = jnp.dot(normed, decay_cols, preferred_element_type=jnp.float32)
    decay = jnp.exp(-decay_rate * jax.nn.softplus(pre_decay + decay_bias))
    strength = jax.nn.sigmoid(jnp.dot(normed, beta_cols, preferred_element_type=jnp.float32))
    rates = jnp.stack([decay, strength], axis=-1).reshape(rows * head_count, 2)
    new_state, head_out = update_state(proj, rates, out_gain[None, :], state)
    head_out = head_out.reshape(rows, head_count * HEAD_DIM)
    partial_value = jnp.dot(head_out, w_out, preferred_element_type=jnp.float32)
    feature_start = lax.axis_index("tp") * width_share
    gain_share = lax.dynamic_slice_in_dim(ffn_gain, feature_start, width_share, 0)
    mixed = channel_mixer(
        partial_value.astype(jnp.bfloat16),
        tokens,
        gain_share[None, :],
        w_up,
        w_down,
        chips,
        groups,
    )
    return (mixed, new_state)


def solution(mesh):
    in_specs = (
        P("kv", "tp"),
        P("kv", "tp", None),
        P(None, "tp"),
        P(None, "tp"),
        P(None, "tp"),
        P(None, "tp"),
        P(),
        P(),
        P("tp"),
        P("tp"),
        P(),
        P(),
        P("tp", None),
        P(),
        P("tp", "kv"),
        P("kv", "tp"),
    )
    out_specs = (P("kv", "tp"), P("kv", "tp", None))
    body = functools.partial(local, mesh.shape["tp"] // CORES, mesh.shape["kv"])
    return jax.shard_map(body, mesh=mesh, in_specs=in_specs, out_specs=out_specs, check_vma=False)
```

```python
import functools

import jax
import jax.numpy as jnp
from jax import lax
from jax.experimental import pallas as pl
from jax.experimental.pallas import tpu as pltpu
from jax.sharding import PartitionSpec as P

HEAD_DIM = 64


EPS = 1e-06


def unit_norm(vector):
    return vector * lax.rsqrt(jnp.sum(vector * vector, axis=-1, keepdims=True) + EPS)


MESH = pl.DeviceIdType.MESH
VMEM = pltpu.VMEM
CORES = 2


def remote(src, dst, send, recv, where):
    return pltpu.make_async_remote_copy(
        src_ref=src, dst_ref=dst, send_sem=send, recv_sem=recv, device_id=where, device_id_type=MESH
    )


def place(chips):
    me = lax.axis_index("tp")
    return lax.div(me, CORES), lax.rem(me, CORES)


def columns(block, width):
    return pl.ds(pl.multiple_of(block * width, 128), width)


def project_kernel(
    chips, x_ref, gain_ref, decay_ref, beta_ref, wq_hbm, wk_hbm, wv_hbm, wg_hbm,
    proj_ref, rate_ref, blocks_ref, w_ref, square_ref, load_sem, own_sem,
    send, recv, pass_send, pass_recv,
):
    f32, bf16 = jnp.float32, jnp.bfloat16
    chip, core = place(chips)
    me = chip * CORES + core
    width = x_ref.shape[1]
    out_width = wq_hbm.shape[1]
    partner = {"tp": chip * CORES + 1 - core}

    def peer(step):
        return {"tp": lax.rem(chip + step, chips) * CORES + core}

    def source(step):
        return lax.rem(chip + chips - step, chips) * CORES

    barrier = pltpu.get_barrier_semaphore()
    pl.semaphore_signal(barrier, inc=1, device_id=partner, device_id_type=MESH)
    for step in range(1, chips):
        pl.semaphore_signal(barrier, inc=1, device_id=peer(step), device_id_type=MESH)
    loads = []
    for i, hbm in enumerate((wq_hbm, wk_hbm, wv_hbm, wg_hbm)):
        there = w_ref.at[:, i * out_width : (i + 1) * out_width]
        loads.append(pltpu.make_async_copy(hbm, there, load_sem.at[i]))
        loads[-1].start()
    keep = pltpu.make_async_copy(x_ref, blocks_ref.at[me], own_sem)
    keep.start()
    proj_ref[...] = jnp.zeros_like(proj_ref)
    rate_ref[...] = jnp.zeros_like(rate_ref)
    square_ref[...] = jnp.zeros_like(square_ref)
    pl.semaphore_wait(barrier, chips)

    def far(step):
        return remote(x_ref, blocks_ref.at[me], send.at[step], recv.at[step], peer(step))

    def passed(step):
        there = blocks_ref.at[source(step) + core]
        return remote(there, there, pass_send.at[step], pass_recv.at[step], partner)

    for step in range(1, chips):
        far(step).start()
    near = remote(x_ref, blocks_ref.at[me], send.at[0], recv.at[0], partner)
    near.start()
    keep.wait()
    for load in loads:
        load.wait()

    def use(block):
        at = columns(block, width)
        raw = blocks_ref[block].astype(f32)
        square_ref[...] += jnp.sum(raw * raw, axis=-1, keepdims=True)
        scaled = (raw * gain_ref[:, at]).astype(bf16)
        proj_ref[...] += jnp.dot(scaled, w_ref[at, :], preferred_element_type=f32)
        rate_ref[0] += jnp.dot(scaled, decay_ref[at, :], preferred_element_type=f32)
        rate_ref[1] += jnp.dot(scaled, beta_ref[at, :], preferred_element_type=f32)

    use(me)
    near.wait_recv()
    use(source(0) + 1 - core)

    @pl.loop(1, chips)
    def _(step):
        far(step).wait_recv()
        passed(step).start()
        use(source(step) + core)

    @pl.loop(1, chips)
    def _(step):
        passed(step).wait_recv()
        use(source(step) + 1 - core)

    scale = lax.rsqrt(square_ref[...] * (1.0 / (width * chips * CORES)) + EPS)
    proj_ref[...] = proj_ref[...] * scale
    rate_ref[0] = rate_ref[0] * scale
    rate_ref[1] = rate_ref[1] * scale
    near.wait_send()

    @pl.loop(1, chips)
    def _(step):
        far(step).wait_send()
        passed(step).wait_send()


def project(tokens, mix_gain, w_decay, w_beta, weights, chips):
    rows, width = tokens.shape
    full, out_width = weights[0].shape
    heads = w_decay.shape[1]
    dma = pltpu.SemaphoreType.DMA
    spec = pl.BlockSpec(memory_space=VMEM)
    return pl.pallas_call(
        functools.partial(project_kernel, chips),
        out_shape=(
            jax.ShapeDtypeStruct((rows, 4 * out_width), jnp.float32),
            jax.ShapeDtypeStruct((2, rows, heads), jnp.float32),
        ),
        in_specs=[spec] * 4 + [pl.BlockSpec(memory_space=pl.ANY)] * 4,
        out_specs=(spec, spec),
        scratch_shapes=[
            VMEM((chips * CORES, rows, width), tokens.dtype),
            VMEM((full, 4 * out_width), jnp.bfloat16),
            VMEM((rows, 1), jnp.float32),
            dma((4,)),
            dma,
        ]
        + [dma((chips,))] * 4,
        compiler_params=pltpu.CompilerParams(
            collective_id=0, has_side_effects=True, vmem_limit_bytes=40 * 1024 * 1024
        ),
        name="project",
    )(tokens, mix_gain, w_decay, w_beta, *weights)


def mixer_kernel(
    chips, groups, part_ref, tok_ref, gain_ref, up_hbm, down_hbm, o_ref,
    up_ref, down_ref, pair_in, pair_sum, chip_in, resid_ref, y_ref, sq_ref,
    up_out, up_in, own_ref, sum_out, from_left, from_right, up_acc, h_ref, acc_ref, d_out, d_in,
    up_load_sem, load_sem, s_pair, r_pair, s_chip, r_chip, s_y, r_y, s_sq, r_sq,
    s_up, r_up, s_sr, r_sr, s_sl, r_sl, s_gr, r_gr, s_gl, r_gl, s_pass, r_pass, s_d, r_d,
):
    chip, core = place(chips)
    me = chip * CORES + core
    group = lax.axis_index("kv")
    ranks = chips * CORES
    rows, width = tok_ref.shape
    hid = up_ref.shape[1] // ranks
    partner = {"tp": chip * CORES + 1 - core}
    f32, bf16 = jnp.float32, jnp.bfloat16

    def ahead(step):
        return lax.rem(chip + step, chips)

    def peer(step):
        return {"tp": ahead(step) * CORES + core}

    def rank_peer(step):
        return {"tp": lax.rem(me + step, ranks)}

    def group_peer(step):
        return {"kv": lax.rem(group + step, groups)}

    barrier = pltpu.get_barrier_semaphore()
    for step in range(1, ranks):
        pl.semaphore_signal(barrier, inc=1, device_id=rank_peer(step), device_id_type=MESH)
    for step in range(1, groups):
        pl.semaphore_signal(barrier, inc=1, device_id=group_peer(step), device_id_type=MESH)
    up_load = pltpu.make_async_copy(up_hbm, up_ref, up_load_sem)
    up_load.start()
    load = pltpu.make_async_copy(down_hbm, down_ref, load_sem)
    load.start()
    pl.semaphore_wait(barrier, ranks + groups - 2)

    order = list(range(1, chips)) + [0]
    pair = {}
    for step in order:
        there = part_ref.at[:, columns(ahead(step) * CORES + 1 - core, width)]
        pair[step] = remote(there, pair_in.at[step], s_pair.at[step], r_pair.at[step], partner)
        pair[step].start()
    far = {}
    for step in order:
        pair[step].wait_recv()
        both = part_ref[:, columns(ahead(step) * CORES + core, width)].astype(f32) + pair_in[
            step
        ].astype(f32)
        if step:
            pair_sum[step] = both.astype(bf16)
            far[step] = remote(
                pair_sum.at[step], chip_in.at[step], s_chip.at[step], r_chip.at[step], peer(step)
            )
            far[step].start()
    resid = tok_ref[...].astype(f32) + both
    for step in range(1, chips):
        far[step].wait_recv()
        resid = resid + chip_in[step].astype(f32)
    resid_ref[...] = resid
    y_ref[0] = (resid * gain_ref[...]).astype(bf16)
    spread = {}
    for step in range(1, groups):
        spread[step] = remote(
            y_ref.at[0], y_ref.at[step], s_y.at[step], r_y.at[step], group_peer(step)
        )
        spread[step].start()
    sq_ref[0] = lax.dot_general(
        jnp.ones((8, width), f32),
        resid * resid,
        (((1,), (1,)), ((), ())),
        precision=lax.Precision.HIGHEST,
        preferred_element_type=f32,
    )
    squares = {}
    for step in range(1, ranks):
        squares[step] = remote(
            sq_ref.at[0], sq_ref.at[step], s_sq.at[step], r_sq.at[step], rank_peer(step)
        )
        squares[step].start()
    for step in range(1, groups):
        spread[step].wait_recv()

    half = groups * rows // 2
    last = chips - 1
    right = {"tp": lax.rem(me + CORES, ranks)}
    left = {"tp": lax.rem(me + ranks - CORES, ranks)}

    def span(part):
        return pl.ds(part * half, half)

    def up_block(part, block):
        wanted = y_ref[part * groups // 2 : (part + 1) * groups // 2]
        return jnp.dot(
            wanted.reshape(half, width),
            up_ref[:, columns(block, hid)],
            preferred_element_type=f32,
        )

    def up_pair(part, t):
        i = part * chips + t
        at = span(part)
        return remote(up_out.at[t, at], up_in.at[t, at], s_up.at[i], r_up.at[i], partner)

    def sum_right(part, t):
        i = part * chips + t
        at = span(part)
        return remote(sum_out.at[t, at], from_left.at[t, at], s_sr.at[i], r_sr.at[i], right)

    def sum_left(part, t):
        i = part * chips + t
        at = span(part)
        return remote(sum_out.at[t, at], from_right.at[t, at], s_sl.at[i], r_sl.at[i], left)

    def block_right(part, t):
        i = part * chips + t
        there = h_ref.at[t * CORES + core, span(part)]
        return remote(there, there, s_gr.at[i], r_gr.at[i], right)

    def block_left(part, t):
        i = part * chips + t
        there = h_ref.at[t * CORES + core, span(part)]
        return remote(there, there, s_gl.at[i], r_gl.at[i], left)

    def block_pass(part, t):
        i = part * chips + t
        there = h_ref.at[t * CORES + core, span(part)]
        return remote(there, there, s_pass.at[i], r_pass.at[i], partner)

    def up(part):
        at = span(part)

        @pl.loop(0, chips)
        def _(t):
            up_out[t, at] = up_block(part, t * CORES + 1 - core).astype(bf16)
            up_pair(part, t).start()

        @pl.loop(0, chips)
        def _(t):
            own = up_block(part, t * CORES + core)
            up_pair(part, t).wait_recv()
            own_ref[t, at] = own + up_in[t, at].astype(f32)

    def sum_step(part, step):
        at = span(part)
        for t, going, first, more, copy, arrived in (
            (last - step, chip < last - step, chip == 0, chip > 0, sum_right, from_left),
            (step, chip > step, chip == last, chip < last, sum_left, from_right),
        ):

            @pl.when(jnp.logical_and(going, first))
            def _():
                sum_out[t, at] = own_ref[t, at].astype(bf16)
                copy(part, t).start()

            @pl.when(jnp.logical_and(going, more))
            def _():
                copy(part, t).wait_recv()
                sum_out[t, at] = (own_ref[t, at] + arrived[t, at].astype(f32)).astype(bf16)
                copy(part, t).start()

    def sum_end(part):
        at = span(part)
        up_acc[...] = own_ref[chip, at]

        @pl.when(chip > 0)
        def _():
            sum_right(part, chip).wait_recv()
            up_acc[...] += from_left[chip, at].astype(f32)

        @pl.when(chip < last)
        def _():
            sum_left(part, chip).wait_recv()
            up_acc[...] += from_right[chip, at].astype(f32)

        h_ref[me, at] = jnp.square(jnp.maximum(up_acc[...], 0.0)).astype(bf16)

        @pl.when(chip < last)
        def _():
            block_right(part, chip).start()

        @pl.when(chip > 0)
        def _():
            block_left(part, chip).start()

        block_pass(part, chip).start()

    def down_add(part, block):
        acc_ref[span(part)] += jnp.dot(
            h_ref[block, span(part)],
            down_ref[pl.ds(pl.multiple_of(block * hid, 128), hid), :],
            preferred_element_type=f32,
        )

    def block_step(part, step, multiply):
        @pl.when(chip >= step)
        def _():
            t = chip - step
            block_right(part, t).wait_recv()

            @pl.when(chip < last)
            def _():
                block_right(part, t).start()

            block_pass(part, t).start()
            if multiply:
                down_add(part, t * CORES + core)

        @pl.when(chip + step <= last)
        def _():
            t = chip + step
            block_left(part, t).wait_recv()

            @pl.when(chip > 0)
            def _():
                block_left(part, t).start()

            block_pass(part, t).start()
            if multiply:
                down_add(part, t * CORES + core)

    up_load.wait()
    up(0)
    sum_step(0, 0)
    up(1)
    acc_ref[...] = jnp.zeros_like(acc_ref)
    for step in range(1, last):
        sum_step(0, step)
    sum_end(0)
    sum_step(1, 0)
    for step in range(1, last):
        block_step(0, step, False)
        sum_step(1, step)
    sum_end(1)
    block_step(0, last, False)
    load.wait()

    @pl.loop(0, chips)
    def _(t):
        down_add(0, t * CORES + core)
        block_pass(0, t).wait_recv()
        down_add(0, t * CORES + 1 - core)

    down_add(1, me)

    @pl.loop(1, chips)
    def _(step):
        block_step(1, step, True)

    @pl.loop(0, chips)
    def _(t):
        block_pass(1, t).wait_recv()
        down_add(1, t * CORES + 1 - core)

    back = {}
    for step in range(1, groups):
        d_out[step] = acc_ref[step * rows : (step + 1) * rows, :].astype(bf16)
        back[step] = remote(
            d_out.at[step], d_in.at[step], s_d.at[step], r_d.at[step], group_peer(groups - step)
        )
        back[step].start()
    for step in range(1, ranks):
        squares[step].wait_recv()
    total = sq_ref[0]
    for step in range(1, ranks):
        total = total + sq_ref[step]
    spots = lax.dot_general(
        total,
        jnp.full((8, width), 0.125, f32),
        (((0,), (0,)), ((), ())),
        precision=lax.Precision.HIGHEST,
        preferred_element_type=f32,
    )
    scale = lax.rsqrt(spots * (1.0 / (width * ranks)) + EPS)
    mixed = acc_ref[0:rows, :]
    for step in range(1, groups):
        back[step].wait_recv()
        mixed = mixed + d_in[step].astype(f32)
    o_ref[...] = (resid_ref[...] + scale * scale * mixed).astype(bf16)

    for copies in (pair, far, spread, squares, back):
        for copy in copies.values():
            copy.wait_send()
    for part in range(2):

        @pl.loop(0, chips)
        def _(t):
            up_pair(part, t).wait_send()
            block_pass(part, t).wait_send()

            @pl.when(t > chip)
            def _():
                sum_right(part, t).wait_send()

            @pl.when(t < chip)
            def _():
                sum_left(part, t).wait_send()

            @pl.when(jnp.logical_and(t <= chip, chip < last))
            def _():
                block_right(part, t).wait_send()

            @pl.when(jnp.logical_and(t >= chip, chip > 0))
            def _():
                block_left(part, t).wait_send()


def channel_mixer(partial_value, tokens, gain_share, w_up, w_down, chips, groups):
    rows, width = tokens.shape
    ranks = chips * CORES
    hid = w_up.shape[1] // ranks
    all_rows = groups * rows
    bf16, f32 = jnp.bfloat16, jnp.float32
    dma = pltpu.SemaphoreType.DMA
    spec = pl.BlockSpec(memory_space=VMEM)
    return pl.pallas_call(
        functools.partial(mixer_kernel, chips, groups),
        out_shape=jax.ShapeDtypeStruct((rows, width), bf16),
        in_specs=[spec] * 3 + [pl.BlockSpec(memory_space=pl.ANY)] * 2,
        out_specs=spec,
        scratch_shapes=[
            VMEM(w_up.shape, bf16),
            VMEM(w_down.shape, bf16),
            VMEM((chips, rows, width), bf16),
            VMEM((chips, rows, width), bf16),
            VMEM((chips, rows, width), bf16),
            VMEM((rows, width), f32),
            VMEM((groups, rows, width), bf16),
            VMEM((ranks, 8, rows), f32),
            VMEM((chips, all_rows, hid), bf16),
            VMEM((chips, all_rows, hid), bf16),
            VMEM((chips, all_rows, hid), f32),
            VMEM((chips, all_rows, hid), bf16),
            VMEM((chips, all_rows, hid), bf16),
            VMEM((chips, all_rows, hid), bf16),
            VMEM((all_rows // 2, hid), f32),
            VMEM((ranks, all_rows, hid), bf16),
            VMEM((all_rows, width), f32),
            VMEM((groups, rows, width), bf16),
            VMEM((groups, rows, width), bf16),
            dma,
            dma,
        ]
        + [dma((chips,))] * 4
        + [dma((groups,))] * 2
        + [dma((ranks,))] * 2
        + [dma((2 * chips,))] * 12
        + [dma((groups,))] * 2,
        compiler_params=pltpu.CompilerParams(
            collective_id=1, has_side_effects=True, vmem_limit_bytes=48 * 1024 * 1024
        ),
        name="channel_mixer",
    )(partial_value, tokens, gain_share, w_up, w_down)


def doubled(x):
    return jnp.concatenate([x, x], axis=-1)


def state_kernel(
    heads, proj_ref, rates_ref, gain_ref, state_ref, new_ref, out_ref,
    spread_ref, wide_ref, val_ref, row_ref, head_ref,
):
    f32, bf16 = jnp.float32, jnp.bfloat16
    lanes = 2 * HEAD_DIM
    count = out_ref.shape[0]
    full = state_ref.shape[2]
    pack = 8 // heads

    @pl.when(pl.program_id(0) == 0)
    def _():
        feature = lax.broadcasted_iota(jnp.int32, spread_ref.shape, 0)
        lane = lax.broadcasted_iota(jnp.int32, spread_ref.shape, 1)
        hit = lax.rem(feature, HEAD_DIM) == lax.div(lane, HEAD_DIM)
        spread_ref[...] = jnp.where(hit, 1.0, 0.0).astype(bf16)

    query = unit_norm(proj_ref[0]) * HEAD_DIM ** (-0.5)
    key_proj = unit_norm(proj_ref[1])
    match = jnp.sum(query * key_proj, axis=-1, keepdims=True)
    both = doubled(jnp.concatenate([key_proj, query], axis=0))
    high = both.astype(bf16).astype(f32)
    rest = both - high
    middle = rest.astype(bf16).astype(f32)
    low = rest - middle
    first = lax.broadcasted_iota(jnp.int32, both.shape, 1) < HEAD_DIM
    parts = jnp.concatenate(
        [jnp.where(first, high, middle), jnp.where(first, low, 0.0)], axis=-1
    ).astype(bf16)
    wide_ref[...] = jnp.dot(parts, spread_ref[...], preferred_element_type=f32)
    val_ref[...] = doubled(proj_ref[2])
    row_ref[0] = jnp.broadcast_to(rates_ref[:, 0:1], (count, lanes))
    row_ref[1] = jnp.broadcast_to(rates_ref[:, 1:2], (count, lanes))
    row_ref[2] = jnp.broadcast_to(match, (count, lanes))

    @pl.loop(0, count // 8)
    def _(index):
        here = pl.ds(pl.multiple_of(index * 8, 8), 8)
        there = pl.ds(pl.multiple_of(index * 8 + count, 8), 8)

        def state_at(at):
            return jnp.concatenate(
                [state_ref[index * pack + i, :, at] for i in range(pack)], axis=0
            )

        by_key = jnp.zeros((8, lanes), f32)
        by_query = jnp.zeros((8, lanes), f32)
        for start in range(0, full, lanes):
            at = slice(start, start + lanes)
            now = state_at(at)
            by_key = by_key + now * wide_ref[here, at]
            by_query = by_query + now * wide_ref[there, at]
        by_key = by_key + pltpu.roll(by_key, HEAD_DIM, 1)
        by_query = by_query + pltpu.roll(by_query, HEAD_DIM, 1)
        decay = row_ref[0, here, :]
        delta = (val_ref[here, :] - decay * by_key) * row_ref[1, here, :]
        head_ref[here, :] = decay * by_query + row_ref[2, here, :] * delta
        for start in range(0, full, lanes):
            at = slice(start, start + lanes)
            new = decay * state_at(at) + wide_ref[here, at] * delta
            for i in range(pack):
                new_ref[index * pack + i, :, at] = new[i * heads : (i + 1) * heads]

    head_out = head_ref[:, 0:HEAD_DIM]
    gate = proj_ref[3]
    out_ref[...] = (
        head_out
        * lax.rsqrt(jnp.mean(head_out * head_out, axis=-1, keepdims=True) + EPS)
        * gain_ref[...]
        * (gate * jax.nn.sigmoid(gate))
    ).astype(bf16)


def update_state(proj, rates, out_gain, state):
    rows, heads, full = state.shape
    block = rows // 3
    count = block * heads
    f32, bf16 = jnp.float32, jnp.bfloat16
    return pl.pallas_call(
        functools.partial(state_kernel, heads),
        grid=(rows // block,),
        out_shape=(
            jax.ShapeDtypeStruct(state.shape, f32),
            jax.ShapeDtypeStruct((rows * heads, HEAD_DIM), bf16),
        ),
        in_specs=[
            pl.BlockSpec((4, count, HEAD_DIM), lambda i: (0, i, 0)),
            pl.BlockSpec((count, 2), lambda i: (i, 0)),
            pl.BlockSpec((1, HEAD_DIM), lambda i: (0, 0)),
            pl.BlockSpec((block, heads, full), lambda i: (i, 0, 0)),
        ],
        out_specs=(
            pl.BlockSpec((block, heads, full), lambda i: (i, 0, 0)),
            pl.BlockSpec((count, HEAD_DIM), lambda i: (i, 0)),
        ),
        scratch_shapes=[
            VMEM((4 * HEAD_DIM, full), bf16),
            VMEM((2 * count, full), f32),
            VMEM((count, 2 * HEAD_DIM), f32),
            VMEM((3, count, 2 * HEAD_DIM), f32),
            VMEM((count, 2 * HEAD_DIM), f32),
        ],
        compiler_params=pltpu.CompilerParams(vmem_limit_bytes=32 * 1024 * 1024),
        name="update_state",
    )(proj, rates, out_gain, state)


def local(
    chips,
    groups,
    tokens,
    state,
    w_query,
    w_key,
    w_value,
    w_gate,
    w_decay,
    w_beta,
    decay_rate,
    decay_bias,
    mix_gain,
    out_gain,
    w_out,
    ffn_gain,
    w_up,
    w_down,
):
    rows = tokens.shape[0]
    width_share = tokens.shape[1]
    head_count = w_query.shape[1] // HEAD_DIM
    proj, rate_rows = project(
        tokens, mix_gain[None, :], w_decay, w_beta, (w_query, w_key, w_value, w_gate), chips
    )
    proj = proj.reshape(rows, 4, head_count, HEAD_DIM).transpose(1, 0, 2, 3)
    proj = proj.reshape(4, rows * head_count, HEAD_DIM)
    head_start = lax.axis_index("tp") * head_count
    rate_rows = lax.dynamic_slice_in_dim(rate_rows, head_start, head_count, 2)
    decay = jnp.exp(-decay_rate * jax.nn.softplus(rate_rows[0] + decay_bias))
    strength = jax.nn.sigmoid(rate_rows[1])
    rates = jnp.stack([decay, strength], axis=-1).reshape(rows * head_count, 2)
    new_state, head_out = update_state(proj, rates, out_gain[None, :], state)
    head_out = head_out.reshape(rows, head_count * HEAD_DIM)
    partial_value = jnp.dot(head_out, w_out, preferred_element_type=jnp.float32)
    feature_start = lax.axis_index("tp") * width_share
    gain_share = lax.dynamic_slice_in_dim(ffn_gain, feature_start, width_share, 0)
    mixed = channel_mixer(
        partial_value.astype(jnp.bfloat16),
        tokens,
        gain_share[None, :],
        w_up,
        w_down,
        chips,
        groups,
    )
    return (mixed, new_state)


def solution(mesh):
    in_specs = (
        P("kv", "tp"),
        P("kv", "tp", None),
        P(None, "tp"),
        P(None, "tp"),
        P(None, "tp"),
        P(None, "tp"),
        P(),
        P(),
        P("tp"),
        P("tp"),
        P(),
        P(),
        P("tp", None),
        P(),
        P("tp", "kv"),
        P("kv", "tp"),
    )
    out_specs = (P("kv", "tp"), P("kv", "tp", None))
    body = functools.partial(local, mesh.shape["tp"] // CORES, mesh.shape["kv"])
    return jax.shard_map(body, mesh=mesh, in_specs=in_specs, out_specs=out_specs, check_vma=False)
```
